32 devices in a mesh: sp: 8 (over z, y), tp: 4 (over x, core).
Axes of the slice: x: 2, y: 2, z: 4, core: 2. Of those that a mesh axis runs over, the one named last changes fastest.
Arguments:
- resid: bfloat16 [2048, 2048], P(('sp', 'tp')), may hold values from -0.21875 to 0.21875
- query_a: bfloat16 [2048, 1024], P('sp', 'tp'), may hold values from -6 to 6
- key_a: bfloat16 [2048, 256], P('sp', 'tp'), may hold values from -6 to 6
- value_a: bfloat16 [2048, 256], P('sp', 'tp'), may hold values from -6 to 6
- query_b: bfloat16 [2048, 1024], P('sp', 'tp'), may hold values from -6 to 6
- key_b: bfloat16 [2048, 512], P('sp', 'tp'), may hold values from -6 to 6
- value_b: bfloat16 [2048, 512], P('sp', 'tp'), may hold values from -6 to 6
- gain_qa: float32 [64], replicated, may hold values from 0.1 to 8
- gain_ka: float32 [64], replicated, may hold values from 0.1 to 8
- gain_qb: float32 [128], replicated, may hold values from 0.1 to 8
- gain_kb: float32 [128], replicated, may hold values from 0.1 to 8
- w_out_a: bfloat16 [1024, 2048], P('tp'), may hold values from -0.125 to 0.125
- w_out_b: bfloat16 [1024, 2048], P('tp'), may hold values from -0.125 to 0.125
- norm_gain: float32 [2048], replicated, may hold values from 0.1 to 1.9
- w_up: bfloat16 [2048, 8192], P('sp', 'tp'), may hold values from -0.125 to 0.125
- w_down: bfloat16 [8192, 2048], P('tp', 'sp'), may hold values from -0.0625 to 0.0625
Outputs:
- result: bfloat16 [2048, 2048], P(('sp', 'tp'))
The draws below stay inside these ranges and needn't reach their ends.
All inputs are finite; a program needn't handle non-finite values.
Results may differ from the reference program's by a relative error of at most 0.02.
The reference program's roundings to bfloat16 on the way count: a program that leaves them out, or rounds other values in their place, can miss the bound.
Values may be sent and summed in bfloat16 or wider, within the bound.
A program may use at most 128 MiB of HBM per device.

```python
import math
import jax
import jax.numpy as jnp
from jax import lax

D = 2048
FF = 8192
HD_A = 64
HD_B = 128
HEADS_A = 16
HEADS_B = 8
KV_A = 4
KV_B = 4
GRID_W = 64
TOKENS = 2048
ATT_W = 2048


def pair_draw(key, heads, kv_heads, width, salt):
    base = jax.random.fold_in(key, salt)
    keys = jnp.clip(jax.random.normal(jax.random.fold_in(base, 1), (TOKENS, kv_heads * width), jnp.float32), -6.0, 6.0)
    queries = jnp.clip(jax.random.normal(jax.random.fold_in(base, 2), (TOKENS, heads * width), jnp.float32), -6.0, 6.0)
    return (queries.astype(jnp.bfloat16), keys.astype(jnp.bfloat16))


def gain_draw(key, width, salt):
    inner = jax.random.fold_in(key, salt)
    return jnp.clip(1.0 + 0.18 * jax.random.normal(inner, (width,), jnp.float32), 0.1, 1.9)


def draw_query_a(key, part):
    return pair_draw(key, HEADS_A, KV_A, HD_A, 101)[0]


def draw_key_a(key, part):
    return pair_draw(key, HEADS_A, KV_A, HD_A, 101)[1]


def draw_query_b(key, part):
    return pair_draw(key, HEADS_B, KV_B, HD_B, 202)[0]


def draw_key_b(key, part):
    return pair_draw(key, HEADS_B, KV_B, HD_B, 202)[1]


def draw_gain_qa(key, part):
    return gain_draw(key, HD_A, 31)


def draw_gain_ka(key, part):
    return gain_draw(key, HD_A, 32)


def draw_gain_qb(key, part):
    return gain_draw(key, HD_B, 33)


def draw_gain_kb(key, part):
    return gain_draw(key, HD_B, 34)


def shard_levels(own_key, extent, pieces, least, high):
    factor_of = 1.0
    for dim, blocks in pieces:
        heights = jax.random.uniform(jax.random.fold_in(jax.random.fold_in(own_key, 6), dim), (blocks,), jnp.float32, least / len(pieces), high / len(pieces))
        factor_of = factor_of * jnp.repeat(jnp.exp(heights), extent[dim] // blocks).reshape((-1,) + (1,) * (len(extent) - 1 - dim))
    return factor_of


def normal_values(rng, extent, scale, reach, cuts=(), kind=jnp.bfloat16):
    entries = jax.random.normal(rng, extent, jnp.float32) * scale
    if len(cuts) > 0:
        entries = shard_levels(rng, extent, cuts, -0.22, 0.18) * entries
    return jnp.clip(entries, min=-reach, max=reach).astype(kind)


def setup_inputs(seed: int = 0) -> dict:
    key_of = jax.random.split(jax.random.key(seed), 17)
    return {
        "resid": normal_values(key_of[0], (TOKENS, D), 0.015, 0.21875, ((0, 32),)),
        "query_a": draw_query_a(jax.random.fold_in(key_of[16], 71), 0),
        "key_a": draw_key_a(jax.random.fold_in(key_of[16], 71), 0),
        "value_a": normal_values(key_of[3], (TOKENS, KV_A * HD_A), 1.0, 6.0, ((0, 8), (1, 4))),
        "query_b": draw_query_b(jax.random.fold_in(key_of[16], 71), 0),
        "key_b": draw_key_b(jax.random.fold_in(key_of[16], 71), 0),
        "value_b": normal_values(key_of[6], (TOKENS, KV_B * HD_B), 1.0, 6.0, ((0, 8), (1, 4))),
        "gain_qa": draw_gain_qa(jax.random.fold_in(key_of[16], 71), 0),
        "gain_ka": draw_gain_ka(jax.random.fold_in(key_of[16], 71), 0),
        "gain_qb": draw_gain_qb(jax.random.fold_in(key_of[16], 71), 0),
        "gain_kb": draw_gain_kb(jax.random.fold_in(key_of[16], 71), 0),
        "w_out_a": normal_values(key_of[11], (HEADS_A * HD_A, D), ATT_W ** -0.5, 0.125, ((0, 4),)),
        "w_out_b": normal_values(key_of[12], (HEADS_B * HD_B, D), ATT_W ** -0.5, 0.125, ((0, 4),)),
        "norm_gain": jnp.clip(1.0 + 0.18 * jax.random.normal(key_of[13], (D,), jnp.float32), 0.1, 1.9),
        "w_up": normal_values(key_of[14], (D, FF), D ** -0.5, 0.125, ((0, 8), (1, 4))),
        "w_down": normal_values(key_of[15], (FF, D), FF ** -0.5, 0.0625, ((0, 4), (1, 8))),
    }


EPS = 1e-06

def tables(count, width):
    pos = jnp.arange(count, dtype=jnp.int32)
    grid_rows = (pos // GRID_W).astype(jnp.float32)
    grid_cols = (pos % GRID_W).astype(jnp.float32)
    quarter = width // 4
    freqs = 10000.0 ** (-(2.0 * jnp.arange(quarter, dtype=jnp.float32)) / (width // 2))
    ang_r = grid_rows[:, None] * freqs
    ang_c = grid_cols[:, None] * freqs
    angles = jnp.concatenate([ang_r, ang_r, ang_c, ang_c], axis=-1)
    return (jnp.cos(angles), jnp.sin(angles))

def norm_rope(values, gain, width):
    count = values.shape[0]
    flat = values.astype(jnp.float32).reshape(count, -1, width)
    flat = flat * lax.rsqrt(lax.optimization_barrier(jnp.mean(flat * flat, axis=-1, keepdims=True)) + EPS) * gain.astype(jnp.float32)
    cosine, sine = tables(count, width)
    one, two, three, four = jnp.split(flat, 4, axis=-1)
    turned = jnp.concatenate([-two, one, -four, three], axis=-1)
    return (flat * cosine[:, None, :] + turned * sine[:, None, :]).astype(jnp.bfloat16)

def attend(queries, keys, values, width):
    count, heads = (queries.shape[0], queries.shape[1])
    kv_heads = keys.shape[1]
    groups = heads // kv_heads
    block = math.gcd(count, 256)
    keys32 = keys.astype(jnp.float32)
    vals32 = values.astype(jnp.float32).reshape(count, kv_heads, width)
    blocks = queries.reshape(count // block, block, kv_heads, groups, width)
    scale = width ** (-0.5)

    def one_block(qblock):
        scores = jnp.einsum('rkgd,pkd->kgrp', qblock.astype(jnp.float32), keys32) * scale
        top = lax.optimization_barrier(jnp.max(scores, axis=-1, keepdims=True))
        expo = jnp.exp(scores - top)
        probs = expo.astype(jnp.bfloat16).astype(jnp.float32)
        summed = jnp.einsum('kgrp,pkd->kgrd', probs, vals32)
        outputs = summed / lax.optimization_barrier(jnp.sum(expo, axis=-1))[..., None]
        return jnp.transpose(outputs, (2, 0, 1, 3)).reshape(block, heads * width).astype(jnp.bfloat16)
    return lax.map(one_block, blocks).reshape(count, heads * width)

def reference(resid, query_a, key_a, value_a, query_b, key_b, value_b, gain_qa, gain_ka, gain_qb, gain_kb, w_out_a, w_out_b, norm_gain, w_up, w_down):
    width_a = gain_qa.shape[0]
    width_b = gain_qb.shape[0]
    attn_a = attend(norm_rope(query_a, gain_qa, width_a), norm_rope(key_a, gain_ka, width_a), value_a, width_a)
    attn_b = attend(norm_rope(query_b, gain_qb, width_b), norm_rope(key_b, gain_kb, width_b), value_b, width_b)
    proj = jnp.dot(attn_a, w_out_a, preferred_element_type=jnp.float32) + jnp.dot(attn_b, w_out_b, preferred_element_type=jnp.float32)
    mid = (resid.astype(jnp.float32) + proj).astype(jnp.bfloat16)
    midf = mid.astype(jnp.float32)
    normed = (midf * lax.rsqrt(lax.optimization_barrier(jnp.mean(midf * midf, axis=-1, keepdims=True)) + EPS) * norm_gain).astype(jnp.bfloat16)
    hidden = jnp.square(jax.nn.relu(jnp.dot(normed, w_up, preferred_element_type=jnp.float32))).astype(jnp.bfloat16)
    return (midf + jnp.dot(hidden, w_down, preferred_element_type=jnp.float32)).astype(jnp.bfloat16)
```

```python
import math

import jax
import jax.numpy as jnp
from jax import lax
from jax.experimental import pallas as pl
from jax.experimental.pallas import tpu as pltpu
from jax.sharding import PartitionSpec as P

GRID_W = 64


EPS = 1e-06


def norm_rope(values, gain, places):
    width = gain.shape[0]
    count = values.shape[0]
    flat = values.astype(jnp.float32).reshape(count, -1, width)
    flat = flat * lax.rsqrt(jnp.mean(flat * flat, axis=-1, keepdims=True) + EPS) * gain
    grid_rows = (places // GRID_W).astype(jnp.float32)
    grid_cols = (places % GRID_W).astype(jnp.float32)
    quarter = width // 4
    freqs = 10000.0 ** (-(2.0 * jnp.arange(quarter, dtype=jnp.float32)) / (width // 2))
    ang_r = grid_rows[:, None] * freqs
    ang_c = grid_cols[:, None] * freqs
    angles = jnp.concatenate([ang_r, ang_r, ang_c, ang_c], axis=-1)
    one, two, three, four = jnp.split(flat, 4, axis=-1)
    turned = jnp.concatenate([-two, one, -four, three], axis=-1)
    return (flat * jnp.cos(angles)[:, None, :] + turned * jnp.sin(angles)[:, None, :]).astype(
        jnp.bfloat16
    )


def fold_block(state, queries, key_block, value_block, scale):
    running, total, accum = state
    scores = (
        jnp.einsum("rkgd,pkd->kgrp", queries, key_block, preferred_element_type=jnp.float32) * scale
    )
    newest = jnp.maximum(running, jnp.max(scores, axis=-1))
    factor = jnp.exp(running - newest)
    expo = jnp.exp(scores - newest[..., None])
    total = total * factor + jnp.sum(expo, axis=-1)
    accum = accum * factor[..., None] + jnp.einsum(
        "kgrp,pkd->kgrd", expo.astype(jnp.bfloat16), value_block, preferred_element_type=jnp.float32
    )
    return (newest, total, accum)


def sweep_keys(state, queries, key_piece, value_piece, scale):
    length = key_piece.shape[0]
    block = math.gcd(length, 2048)
    blocks = length // block
    if blocks == 1:
        return fold_block(state, queries, key_piece, value_piece, scale)
    key_blocks = key_piece.reshape((blocks, block) + key_piece.shape[1:])
    value_blocks = value_piece.reshape((blocks, block) + value_piece.shape[1:])

    def advance(carry, pair):
        return (fold_block(carry, queries, pair[0], pair[1], scale), None)

    state, unused = lax.scan(advance, state, (key_blocks, value_blocks))
    return state


def start_state(queries):
    shape = (queries.shape[1], queries.shape[2], queries.shape[0])
    return (
        jnp.full(shape, -1e30, jnp.float32),
        jnp.zeros(shape, jnp.float32),
        jnp.zeros(shape + (queries.shape[3],), jnp.float32),
    )


def finish(state):
    running, total, accum = state
    outputs = accum / total[..., None]
    count = outputs.shape[2]
    return jnp.transpose(outputs, (2, 0, 1, 3)).reshape(count, -1).astype(jnp.bfloat16)


def local(
    resid,
    query_a,
    key_a,
    value_a,
    query_b,
    key_b,
    value_b,
    gain_qa,
    gain_ka,
    gain_qb,
    gain_kb,
    w_out_a,
    w_out_b,
    norm_gain,
    w_up,
    w_down,
):
    count = query_a.shape[0]
    width_a = gain_qa.shape[0]
    width_b = gain_qb.shape[0]
    places = lax.axis_index("sp") * count + jnp.arange(count, dtype=jnp.int32)
    keys_a = norm_rope(key_a, gain_ka, places)
    keys_b = norm_rope(key_b, gain_kb, places)
    heads_kv_a = keys_a.shape[1]
    heads_kv_b = keys_b.shape[1]
    queries_a = norm_rope(query_a, gain_qa, places)
    queries_b = norm_rope(query_b, gain_qb, places)
    queries_a = queries_a.reshape(count, heads_kv_a, queries_a.shape[1] // heads_kv_a, width_a)
    queries_b = queries_b.reshape(count, heads_kv_b, queries_b.shape[1] // heads_kv_b, width_b)
    values_a = value_a.reshape(count, heads_kv_a, width_a)
    values_b = value_b.reshape(count, heads_kv_b, width_b)
    state_a = sweep_keys(
        start_state(queries_a),
        queries_a,
        lax.all_gather(keys_a, "sp", axis=0, tiled=True),
        lax.all_gather(values_a, "sp", axis=0, tiled=True),
        width_a ** (-0.5),
    )
    state_b = sweep_keys(
        start_state(queries_b),
        queries_b,
        lax.all_gather(keys_b, "sp", axis=0, tiled=True),
        lax.all_gather(values_b, "sp", axis=0, tiled=True),
        width_b ** (-0.5),
    )
    attn_a = finish(state_a)
    attn_b = finish(state_b)
    rows_a, rows_b = (
        lax.all_to_all(attn_a, "tp", split_axis=0, concat_axis=1, tiled=True),
        lax.all_to_all(attn_b, "tp", split_axis=0, concat_axis=1, tiled=True),
    )
    whole_a, whole_b = (
        lax.all_gather(w_out_a, "tp", axis=0, tiled=True),
        lax.all_gather(w_out_b, "tp", axis=0, tiled=True),
    )
    proj = jnp.dot(rows_a, whole_a, preferred_element_type=jnp.float32) + jnp.dot(
        rows_b, whole_b, preferred_element_type=jnp.float32
    )
    mid = (resid.astype(jnp.float32) + proj).astype(jnp.bfloat16)
    midf = mid.astype(jnp.float32)
    normed = (
        midf * lax.rsqrt(jnp.mean(midf * midf, axis=-1, keepdims=True) + EPS) * norm_gain
    ).astype(jnp.bfloat16)
    up_whole, down_whole = (
        lax.all_gather(w_up, "sp", axis=0, tiled=True),
        lax.all_gather(w_down, "sp", axis=1, tiled=True),
    )
    hidden = jnp.square(
        jax.nn.relu(
            jnp.dot(
                lax.all_gather(normed, "tp", axis=0, tiled=True),
                up_whole,
                preferred_element_type=jnp.float32,
            )
        )
    ).astype(jnp.bfloat16)
    mixed = lax.psum_scatter(
        jnp.dot(hidden, down_whole, preferred_element_type=jnp.float32).astype(jnp.bfloat16),
        "tp",
        scatter_dimension=0,
        tiled=True,
    ).astype(jnp.float32)
    return (midf + mixed).astype(jnp.bfloat16)


MESH = pl.DeviceIdType.MESH
INNER = 2
LANES = 128


def remote(src, dst, send, recv, target):
    return pltpu.make_async_remote_copy(
        src_ref=src,
        dst_ref=dst,
        send_sem=send,
        recv_sem=recv,
        device_id=target,
        device_id_type=MESH,
    )


def greet(targets):
    barrier = pltpu.get_barrier_semaphore()
    for target in targets:
        pl.semaphore_signal(barrier, inc=1, device_id=target, device_id_type=MESH)
    pl.semaphore_wait(barrier, len(targets))


def exchange_kernel(outer, kv, up, down, kv_all, up_all, down_all, send, recv, here):
    sp = lax.axis_index("sp")
    z = sp // INNER
    y = sp % INNER
    rows = up.shape[0]
    cols = down.shape[1]
    units = up_all.shape[1]
    z_peers = [lax.rem(z + d, outer) for d in range(1, outer)]
    y_peers = [lax.rem(y + d, INNER) for d in range(1, INNER)]
    greet([{"sp": p * INNER + y} for p in z_peers] + [{"sp": z * INNER + p} for p in y_peers])

    def piece(m, target):
        at = pl.ds(pl.multiple_of(target * units, units), units)
        if m == 0:
            return kv
        return up.at[:, at] if m == 1 else down.at[at, :]

    def place(m, source):
        if m == 0:
            return kv_all.at[source]
        if m == 1:
            return up_all.at[pl.ds(pl.multiple_of(source * rows, rows), rows), :]
        return down_all.at[:, pl.ds(pl.multiple_of(source * cols, cols), cols)]

    started = []

    def ship(m, slot, src, source, target):
        copy = remote(src, place(m, source), send.at[m, slot], recv.at[m, source], target)
        copy.start()
        started.append(copy)

    own = []
    for m in range(3):
        for i, p in enumerate(z_peers):
            ship(m, i, piece(m, p), sp, {"sp": p * INNER + y})
        for i, p in enumerate(y_peers):
            ship(m, outer - 1 + i, piece(m, z), sp, {"sp": z * INNER + p})
        copy = pltpu.make_async_copy(piece(m, z), place(m, sp), here.at[m])
        copy.start()
        own.append(copy)
    for m in range(3):
        for d in range(1, outer):
            source = lax.rem(z + outer - d, outer) * INNER + y
            pltpu.make_async_copy(place(m, source), place(m, source), recv.at[m, source]).wait()
            for i, p in enumerate(y_peers):
                ship(
                    m,
                    outer - 1 + d * (INNER - 1) + i,
                    place(m, source),
                    source,
                    {"sp": z * INNER + p},
                )
    for m in range(3):
        for p in y_peers:
            for zs in range(outer):
                source = zs * INNER + p
                pltpu.make_async_copy(place(m, source), place(m, source), recv.at[m, source]).wait()
    for copy in own:
        copy.wait()
    for copy in started:
        copy.wait_send()


def exchange(kv, up, down, total):
    outer = total // INNER
    units = up.shape[1] // outer
    vmem = pl.BlockSpec(memory_space=pltpu.VMEM)
    return pl.pallas_call(
        lambda *refs: exchange_kernel(outer, *refs),
        out_shape=(
            jax.ShapeDtypeStruct((total,) + kv.shape, kv.dtype),
            jax.ShapeDtypeStruct((up.shape[0] * total, units), up.dtype),
            jax.ShapeDtypeStruct((units, down.shape[1] * total), down.dtype),
        ),
        in_specs=[vmem] * 3,
        out_specs=(vmem,) * 3,
        scratch_shapes=[
            pltpu.SemaphoreType.DMA((3, total)),
            pltpu.SemaphoreType.DMA((3, total)),
            pltpu.SemaphoreType.DMA((3,)),
        ],
        compiler_params=pltpu.CompilerParams(
            collective_id=0, has_side_effects=True, vmem_limit_bytes=40 * 1024 * 1024
        ),
        name="exchange",
    )(kv, up, down)


def tail_kernel(
    outer,
    sides,
    steps,
    part,
    resid,
    gain,
    up,
    down,
    out,
    part_in,
    tokens,
    hidden,
    core_out,
    core_in,
    side_out,
    side_in,
    ring_out,
    ring_in,
    keep,
    mid,
    s_part,
    r_part,
    s_tok,
    r_tok,
    s_core,
    r_core,
    s_side,
    r_side,
    s_ring,
    r_ring,
):
    sp = lax.axis_index("sp")
    tp = lax.axis_index("tp")
    z = sp // INNER
    y = sp % INNER
    x = tp // INNER
    c = tp % INNER
    lanes = sides * INNER
    rows, width = resid.shape
    step = width // steps
    f32 = jnp.float32
    z_peers = [lax.rem(z + d, outer) for d in range(1, outer)]
    x_peers = [lax.rem(x + d, sides) for d in range(1, sides)]
    other = 1 - c
    tp_peers = [lax.rem(tp + d, lanes) for d in range(1, lanes)]
    greet([{"sp": p * INNER + y} for p in z_peers] + [{"tp": p} for p in tp_peers])
    started = []

    def ship(src, dst, send, recv, target):
        copy = remote(src, dst, send, recv, target)
        copy.start()
        started.append(copy)

    def arrive(dst, sem):
        pltpu.make_async_copy(dst, dst, sem).wait()

    for i, p in enumerate(tp_peers):
        ship(part.at[p], part_in.at[tp], s_part.at[i], r_part.at[tp], {"tp": p})
    total = resid[...].astype(f32) + part[tp].astype(f32)
    for d in range(1, lanes):
        p = lax.rem(tp + lanes - d, lanes)
        arrive(part_in.at[p], r_part.at[p])
        total = total + part_in[p].astype(f32)
    mid[...] = total.astype(jnp.bfloat16)
    midf = mid[...].astype(f32)
    norm = midf * lax.rsqrt(jnp.mean(midf * midf, axis=-1, keepdims=True) + EPS) * gain[...]
    tokens[tp, z] = norm.astype(jnp.bfloat16)

    sent = [0]

    def pass_on(lane, zs, target):
        ship(
            tokens.at[lane, zs], tokens.at[lane, zs], s_tok.at[sent[0]], r_tok.at[lane, zs], target
        )
        sent[0] += 1

    for p in z_peers:
        pass_on(tp, z, {"sp": p * INNER + y})
    for p in x_peers:
        pass_on(tp, z, {"tp": p * INNER + c})
    pass_on(tp, z, {"tp": x * INNER + other})
    for d in range(1, outer):
        zs = lax.rem(z + outer - d, outer)
        arrive(tokens.at[tp, zs], r_tok.at[tp, zs])
        for p in x_peers:
            pass_on(tp, zs, {"tp": p * INNER + c})
        pass_on(tp, zs, {"tp": x * INNER + other})

    def feed(lane):
        block = tokens[lane].reshape(outer * rows, width)
        made = jnp.maximum(jnp.dot(block, up[...], preferred_element_type=f32), 0.0)
        hidden[lane] = (made * made).astype(jnp.bfloat16)

    feed(tp)
    for d in range(1, sides):
        lane = lax.rem(x + sides - d, sides) * INNER + c
        for e in range(outer):
            zs = lax.rem(z + e, outer)
            arrive(tokens.at[lane, zs], r_tok.at[lane, zs])
            pass_on(lane, zs, {"tp": x * INNER + other})
        feed(lane)
    for d in range(sides):
        lane = lax.rem(x + d, sides) * INNER + other
        for zs in range(outer):
            arrive(tokens.at[lane, zs], r_tok.at[lane, zs])
        feed(lane)

    def product(lane, at):
        return jnp.dot(hidden[lane], down[:, at], preferred_element_type=f32)

    cuts = [pl.ds(j * step, step) for j in range(steps)]
    for j, at in enumerate(cuts):
        for d in list(range(1, sides)) + [0]:
            side = lax.rem(x + d, sides)
            core_out[side, :, at] = product(side * INNER + other, at).astype(jnp.bfloat16)
            ship(
                core_out.at[side, :, at],
                core_in.at[side, :, at],
                s_core.at[side, j],
                r_core.at[side, j],
                {"tp": x * INNER + other},
            )
        for d in list(range(1, sides)) + [0]:
            side = lax.rem(x + d, sides)
            value = product(side * INNER + c, at)
            arrive(core_in.at[side, :, at], r_core.at[side, j])
            value = value + core_in[side, :, at].astype(f32)
            if d == 0:
                keep[:, at] = value
            else:
                side_out[d - 1, :, at] = value.astype(jnp.bfloat16)
                ship(
                    side_out.at[d - 1, :, at],
                    side_in.at[d - 1, :, at],
                    s_side.at[d - 1, j],
                    r_side.at[d - 1, j],
                    {"tp": side * INNER + c},
                )
    for j, at in enumerate(cuts):
        value = keep[:, at]
        for d in range(1, sides):
            arrive(side_in.at[d - 1, :, at], r_side.at[d - 1, j])
            value = value + side_in[d - 1, :, at].astype(f32)
        ring_out[:, :, at] = value.astype(jnp.bfloat16).reshape(outer, rows, step)
        for i, p in enumerate(z_peers):
            ship(
                ring_out.at[p, :, at],
                ring_in.at[i, :, at],
                s_ring.at[i, j],
                r_ring.at[i, j],
                {"sp": p * INNER + y},
            )
    for j, at in enumerate(cuts):
        value = mid[:, at].astype(f32) + ring_out[z, :, at].astype(f32)
        for i in range(outer - 1):
            arrive(ring_in.at[i, :, at], r_ring.at[i, j])
            value = value + ring_in[i, :, at].astype(f32)
        out[:, at] = value.astype(out.dtype)
    for copy in started:
        copy.wait_send()


def tail(part, resid, gain, up, down, total, lanes):
    outer = total // INNER
    sides = lanes // INNER
    rows, width = resid.shape
    steps = 4 if width % (4 * LANES) == 0 else 1
    units = up.shape[1]
    band = outer * rows
    kind = jnp.bfloat16
    vmem = pl.BlockSpec(memory_space=pltpu.VMEM)
    sems = pltpu.SemaphoreType.DMA
    moves = outer - 1 + (sides - 1) * outer + outer + (sides - 1) * outer
    near = max(sides - 1, 1)
    return pl.pallas_call(
        lambda *refs: tail_kernel(outer, sides, steps, *refs),
        out_shape=jax.ShapeDtypeStruct(resid.shape, resid.dtype),
        in_specs=[vmem] * 5,
        out_specs=vmem,
        scratch_shapes=[
            pltpu.VMEM((lanes, rows, width), kind),
            pltpu.VMEM((lanes, outer, rows, width), kind),
            pltpu.VMEM((lanes, band, units), kind),
            pltpu.VMEM((sides, band, width), kind),
            pltpu.VMEM((sides, band, width), kind),
            pltpu.VMEM((near, band, width), kind),
            pltpu.VMEM((near, band, width), kind),
            pltpu.VMEM((outer, rows, width), kind),
            pltpu.VMEM((outer - 1, rows, width), kind),
            pltpu.VMEM((band, width), jnp.float32),
            pltpu.VMEM((rows, width), kind),
            sems((lanes - 1,)),
            sems((lanes,)),
            sems((moves,)),
            sems((lanes, outer)),
            sems((sides, steps)),
            sems((sides, steps)),
            sems((near, steps)),
            sems((near, steps)),
            sems((outer - 1, steps)),
            sems((outer - 1, steps)),
        ],
        compiler_params=pltpu.CompilerParams(
            collective_id=1, has_side_effects=True, vmem_limit_bytes=56 * 1024 * 1024
        ),
        name="tail",
    )(part, resid, gain, up, down)


def kernel_local(
    total,
    lanes,
    resid,
    query_a,
    key_a,
    value_a,
    query_b,
    key_b,
    value_b,
    gain_qa,
    gain_ka,
    gain_qb,
    gain_kb,
    w_out_a,
    w_out_b,
    norm_gain,
    w_up,
    w_down,
):
    count = query_a.shape[0]
    width_a = gain_qa.shape[0]
    width_b = gain_qb.shape[0]
    places = lax.axis_index("sp") * count + jnp.arange(count, dtype=jnp.int32)
    keys_a = norm_rope(key_a, gain_ka, places).reshape(count, -1)
    keys_b = norm_rope(key_b, gain_kb, places).reshape(count, -1)
    kv = jnp.concatenate([keys_b, value_b, keys_a, value_a], axis=1)
    kv_all, up, down = exchange(kv, w_up, w_down, total)
    kv_all = kv_all.reshape(total * count, -1)
    span_a = key_a.shape[1]
    span_b = key_b.shape[1]
    cuts = (span_b, 2 * span_b, 2 * span_b + span_a)
    all_kb, all_vb, all_ka, all_va = jnp.split(kv_all, cuts, axis=1)
    queries_a = norm_rope(query_a, gain_qa, places)
    queries_b = norm_rope(query_b, gain_qb, places)

    def attend(queries, keys, values, width):
        keys = keys.reshape(keys.shape[0], -1, width)
        values = values.reshape(values.shape[0], -1, width)
        heads = keys.shape[1]
        queries = queries.reshape(count, heads, queries.shape[1] // heads, width)
        state = sweep_keys(start_state(queries), queries, keys, values, width ** (-0.5))
        return finish(state)

    attn_a = attend(queries_a, all_ka, all_va, width_a)
    attn_b = attend(queries_b, all_kb, all_vb, width_b)
    part = jnp.dot(attn_a, w_out_a, preferred_element_type=jnp.float32) + jnp.dot(
        attn_b, w_out_b, preferred_element_type=jnp.float32
    )
    part = part.astype(jnp.bfloat16).reshape((lanes,) + resid.shape)
    return tail(part, resid, norm_gain.reshape(1, -1), up, down, total, lanes)


def fits(total, lanes, w_up, w_down):
    if total % INNER or lanes % INNER or total // INNER < 2 or lanes // INNER < 2:
        return False
    units = w_up.shape[1] // lanes // (total // INNER)
    rows = w_up.shape[0] // total
    cols = w_down.shape[1] // total
    small = 2 * units * w_up.shape[0] * 2 <= 8 * 1024 * 1024
    return units % LANES == 0 and rows % 16 == 0 and cols % LANES == 0 and small


def sharded(inside, mesh):
    return jax.shard_map(
        inside,
        mesh=mesh,
        in_specs=(
            P(("sp", "tp"), None),
            P("sp", "tp"),
            P("sp", "tp"),
            P("sp", "tp"),
            P("sp", "tp"),
            P("sp", "tp"),
            P("sp", "tp"),
            P(),
            P(),
            P(),
            P(),
            P("tp", None),
            P("tp", None),
            P(),
            P("sp", "tp"),
            P("tp", "sp"),
        ),
        out_specs=P(("sp", "tp"), None),
        check_vma=False,
    )


def solution(mesh):
    total = mesh.shape["sp"]
    lanes = mesh.shape["tp"]

    def run(*args):
        inside = local
        if fits(total, lanes, args[-2], args[-1]):
            inside = lambda *shards: kernel_local(total, lanes, *shards)
        return sharded(inside, mesh)(*args)

    return run
```

```python
import math

import jax
import jax.numpy as jnp
from jax import lax
from jax.experimental import pallas as pl
from jax.experimental.pallas import tpu as pltpu
from jax.sharding import PartitionSpec as P

GRID_W = 64


EPS = 1e-06


def norm_rope(values, gain, places):
    width = gain.shape[0]
    count = values.shape[0]
    flat = values.astype(jnp.float32).reshape(count, -1, width)
    flat = flat * lax.rsqrt(jnp.mean(flat * flat, axis=-1, keepdims=True) + EPS) * gain
    grid_rows = (places // GRID_W).astype(jnp.float32)
    grid_cols = (places % GRID_W).astype(jnp.float32)
    quarter = width // 4
    freqs = 10000.0 ** (-(2.0 * jnp.arange(quarter, dtype=jnp.float32)) / (width // 2))
    ang_r = grid_rows[:, None] * freqs
    ang_c = grid_cols[:, None] * freqs
    angles = jnp.concatenate([ang_r, ang_r, ang_c, ang_c], axis=-1)
    one, two, three, four = jnp.split(flat, 4, axis=-1)
    turned = jnp.concatenate([-two, one, -four, three], axis=-1)
    return (flat * jnp.cos(angles)[:, None, :] + turned * jnp.sin(angles)[:, None, :]).astype(
        jnp.bfloat16
    )


def fold_block(state, queries, key_block, value_block, scale):
    running, total, accum = state
    scores = (
        jnp.einsum("rkgd,pkd->kgrp", queries, key_block, preferred_element_type=jnp.float32) * scale
    )
    newest = jnp.maximum(running, jnp.max(scores, axis=-1))
    factor = jnp.exp(running - newest)
    expo = jnp.exp(scores - newest[..., None])
    total = total * factor + jnp.sum(expo, axis=-1)
    accum = accum * factor[..., None] + jnp.einsum(
        "kgrp,pkd->kgrd", expo.astype(jnp.bfloat16), value_block, preferred_element_type=jnp.float32
    )
    return (newest, total, accum)


def sweep_keys(state, queries, key_piece, value_piece, scale):
    length = key_piece.shape[0]
    block = math.gcd(length, 2048)
    blocks = length // block
    if blocks == 1:
        return fold_block(state, queries, key_piece, value_piece, scale)
    key_blocks = key_piece.reshape((blocks, block) + key_piece.shape[1:])
    value_blocks = value_piece.reshape((blocks, block) + value_piece.shape[1:])

    def advance(carry, pair):
        return (fold_block(carry, queries, pair[0], pair[1], scale), None)

    state, unused = lax.scan(advance, state, (key_blocks, value_blocks))
    return state


def start_state(queries):
    shape = (queries.shape[1], queries.shape[2], queries.shape[0])
    return (
        jnp.full(shape, -1e30, jnp.float32),
        jnp.zeros(shape, jnp.float32),
        jnp.zeros(shape + (queries.shape[3],), jnp.float32),
    )


def finish(state):
    running, total, accum = state
    outputs = accum / total[..., None]
    count = outputs.shape[2]
    return jnp.transpose(outputs, (2, 0, 1, 3)).reshape(count, -1).astype(jnp.bfloat16)


def local(
    resid,
    query_a,
    key_a,
    value_a,
    query_b,
    key_b,
    value_b,
    gain_qa,
    gain_ka,
    gain_qb,
    gain_kb,
    w_out_a,
    w_out_b,
    norm_gain,
    w_up,
    w_down,
):
    count = query_a.shape[0]
    width_a = gain_qa.shape[0]
    width_b = gain_qb.shape[0]
    places = lax.axis_index("sp") * count + jnp.arange(count, dtype=jnp.int32)
    keys_a = norm_rope(key_a, gain_ka, places)
    keys_b = norm_rope(key_b, gain_kb, places)
    heads_kv_a = keys_a.shape[1]
    heads_kv_b = keys_b.shape[1]
    queries_a = norm_rope(query_a, gain_qa, places)
    queries_b = norm_rope(query_b, gain_qb, places)
    queries_a = queries_a.reshape(count, heads_kv_a, queries_a.shape[1] // heads_kv_a, width_a)
    queries_b = queries_b.reshape(count, heads_kv_b, queries_b.shape[1] // heads_kv_b, width_b)
    values_a = value_a.reshape(count, heads_kv_a, width_a)
    values_b = value_b.reshape(count, heads_kv_b, width_b)
    state_a = sweep_keys(
        start_state(queries_a),
        queries_a,
        lax.all_gather(keys_a, "sp", axis=0, tiled=True),
        lax.all_gather(values_a, "sp", axis=0, tiled=True),
        width_a ** (-0.5),
    )
    state_b = sweep_keys(
        start_state(queries_b),
        queries_b,
        lax.all_gather(keys_b, "sp", axis=0, tiled=True),
        lax.all_gather(values_b, "sp", axis=0, tiled=True),
        width_b ** (-0.5),
    )
    attn_a = finish(state_a)
    attn_b = finish(state_b)
    rows_a, rows_b = (
        lax.all_to_all(attn_a, "tp", split_axis=0, concat_axis=1, tiled=True),
        lax.all_to_all(attn_b, "tp", split_axis=0, concat_axis=1, tiled=True),
    )
    whole_a, whole_b = (
        lax.all_gather(w_out_a, "tp", axis=0, tiled=True),
        lax.all_gather(w_out_b, "tp", axis=0, tiled=True),
    )
    proj = jnp.dot(rows_a, whole_a, preferred_element_type=jnp.float32) + jnp.dot(
        rows_b, whole_b, preferred_element_type=jnp.float32
    )
    mid = (resid.astype(jnp.float32) + proj).astype(jnp.bfloat16)
    midf = mid.astype(jnp.float32)
    normed = (
        midf * lax.rsqrt(jnp.mean(midf * midf, axis=-1, keepdims=True) + EPS) * norm_gain
    ).astype(jnp.bfloat16)
    up_whole, down_whole = (
        lax.all_gather(w_up, "sp", axis=0, tiled=True),
        lax.all_gather(w_down, "sp", axis=1, tiled=True),
    )
    hidden = jnp.square(
        jax.nn.relu(
            jnp.dot(
                lax.all_gather(normed, "tp", axis=0, tiled=True),
                up_whole,
                preferred_element_type=jnp.float32,
            )
        )
    ).astype(jnp.bfloat16)
    mixed = lax.psum_scatter(
        jnp.dot(hidden, down_whole, preferred_element_type=jnp.float32).astype(jnp.bfloat16),
        "tp",
        scatter_dimension=0,
        tiled=True,
    ).astype(jnp.float32)
    return (midf + mixed).astype(jnp.bfloat16)


MESH = pl.DeviceIdType.MESH
INNER = 2
LANES = 128


def remote(src, dst, send, recv, target):
    return pltpu.make_async_remote_copy(
        src_ref=src,
        dst_ref=dst,
        send_sem=send,
        recv_sem=recv,
        device_id=target,
        device_id_type=MESH,
    )


def greet(targets):
    barrier = pltpu.get_barrier_semaphore()
    for target in targets:
        pl.semaphore_signal(barrier, inc=1, device_id=target, device_id_type=MESH)
    pl.semaphore_wait(barrier, len(targets))


def flip(place, k):
    bit = 1
    while bit <= k:
        if k & bit:
            place = place + bit - 2 * bit * lax.rem(place // bit, 2)
        bit *= 2
    return place


def peers_of(place, count):
    return [flip(place, k) for k in range(count - 1, 0, -1)]


def arrive(dst, sem):
    pltpu.make_async_copy(dst, dst, sem).wait()


def front_kernel(
    outer,
    lanes,
    scales,
    kv_in,
    q_a,
    q_b,
    table,
    gains,
    resid,
    norm_gain,
    out_a,
    out_b,
    up,
    down,
    up_all,
    down_all,
    mid,
    normed,
    kv,
    kv_all,
    attn,
    part,
    part_in,
    send,
    recv,
    here,
    s_part,
    r_part,
):
    f32 = jnp.float32
    sp = lax.axis_index("sp")
    tp = lax.axis_index("tp")
    z = sp // INNER
    y = sp % INNER
    rows = up.shape[0]
    cols = down.shape[1]
    units = up_all.shape[1]
    count = q_a.shape[0]
    total = outer * INNER
    z_peers = peers_of(z, outer)
    y_peers = peers_of(y, INNER)
    tp_peers = peers_of(tp, lanes)
    greet(
        [{"sp": p * INNER + y} for p in z_peers]
        + [{"sp": z * INNER + p} for p in y_peers]
        + [{"tp": p} for p in tp_peers]
    )
    lane = lax.broadcasted_iota(jnp.int32, (count, LANES), 1)
    low = lane < LANES // 2

    def spin(value, quarter):
        even = lax.rem(lane // quarter, 2) == 0
        ahead = pltpu.roll(value, LANES - quarter, 1)
        behind = pltpu.roll(value, quarter, 1)
        return jnp.where(even, -ahead, behind)

    def turn_b(raw, gain):
        value = raw.astype(f32)
        value = value * lax.rsqrt(jnp.mean(value * value, axis=-1, keepdims=True) + EPS) * gain
        return value * table[:, 0:LANES] + spin(value, LANES // 4) * table[:, LANES : 2 * LANES]

    def turn_a(raw, gain):
        value = raw.astype(f32)
        square = value * value
        first = jnp.sum(jnp.where(low, square, 0.0), axis=-1, keepdims=True)
        second = jnp.sum(jnp.where(low, 0.0, square), axis=-1, keepdims=True)
        mean = jnp.where(low, first, second) * (2.0 / LANES)
        value = value * lax.rsqrt(mean + EPS) * gain
        cosine = table[:, 2 * LANES : 3 * LANES]
        sine = table[:, 3 * LANES : 4 * LANES]
        return value * cosine + spin(value, LANES // 8) * sine

    raw = kv_in[:, 2 * LANES : 3 * LANES]
    keys = turn_a(raw, gains[3:4, :])
    kv[:, 2 * LANES : 3 * LANES] = jnp.where(low, keys, raw.astype(f32)).astype(jnp.bfloat16)
    kv[:, 0:LANES] = turn_b(kv_in[:, 0:LANES], gains[1:2, :]).astype(jnp.bfloat16)
    kv[:, LANES : 2 * LANES] = kv_in[:, LANES : 2 * LANES]

    def piece(m, target):
        at = pl.ds(pl.multiple_of(target * units, units), units)
        if m == 0:
            return kv
        return up.at[:, at] if m == 1 else down.at[at, :]

    def place(m, source):
        if m == 0:
            return kv_all.at[source]
        if m == 1:
            return up_all.at[pl.ds(pl.multiple_of(source * rows, rows), rows), :]
        return down_all.at[:, pl.ds(pl.multiple_of(source * cols, cols), cols)]

    started = []

    def ship(m, slot, src, source, target):
        copy = remote(src, place(m, source), send.at[m, slot], recv.at[m, source], target)
        copy.start()
        started.append(copy)

    def open_z(m):
        for i, p in enumerate(z_peers):
            ship(m, i, piece(m, p), sp, {"sp": p * INNER + y})

    def open_y(m):
        for i, p in enumerate(y_peers):
            ship(m, outer - 1 + i, piece(m, z), sp, {"sp": z * INNER + p})

    def forward(m, i):
        source = z_peers[i] * INNER + y
        arrive(place(m, source), recv.at[m, source])
        for n, p in enumerate(y_peers):
            slot = outer - 1 + (i + 1) * (INNER - 1) + n
            ship(m, slot, place(m, source), source, {"sp": z * INNER + p})

    def settle(m):
        for p in y_peers:
            for zs in range(outer):
                source = zs * INNER + p
                arrive(place(m, source), recv.at[m, source])

    own = []
    open_z(0)
    open_y(0)
    for m in (1, 2):
        open_z(m)
    open_y(1)
    for m in range(3):
        copy = pltpu.make_async_copy(piece(m, z), place(m, sp), here.at[m])
        copy.start()
        own.append(copy)
    wide = q_a.shape[1] // LANES
    tall = q_b.shape[1] // LANES
    turned_a = []
    turned_b = []
    for n in range(wide):
        value = turn_a(q_a[:, n * LANES : (n + 1) * LANES], gains[2:3, :])
        other = pltpu.roll(value, LANES // 2, 1)
        for v in (value, other):
            turned_a.append(jnp.where(low, v, 0.0).astype(jnp.bfloat16))
    for n in range(tall):
        value = turn_b(q_b[:, n * LANES : (n + 1) * LANES], gains[0:1, :])
        turned_b.append(value.astype(jnp.bfloat16))
    for i in range(outer - 1):
        forward(0, i)
    open_y(2)
    own[0].wait()
    settle(0)

    def attend(query, keys, values, scale):
        scores = lax.dot_general(
            query, keys, (((1,), (1,)), ((), ())), preferred_element_type=f32
        )
        scores = scores * scale
        expo = jnp.exp(scores - jnp.max(scores, axis=-1, keepdims=True))
        summed = jnp.dot(expo.astype(jnp.bfloat16), values, preferred_element_type=f32)
        return summed / jnp.sum(expo, axis=-1, keepdims=True)

    both = kv_all[:, :, 2 * LANES : 3 * LANES].reshape(total * count, LANES)
    for n in range(wide):
        first = attend(turned_a[2 * n], both, both, scales[0])
        second = attend(turned_a[2 * n + 1], both, both, scales[0])
        pair = jnp.where(low, pltpu.roll(first, LANES // 2, 1), second)
        attn[:, n * LANES : (n + 1) * LANES] = pair.astype(jnp.bfloat16)
    forward(1, 0)
    keys = kv_all[:, :, 0:LANES].reshape(total * count, LANES)
    values = kv_all[:, :, LANES : 2 * LANES].reshape(total * count, LANES)
    for n in range(tall):
        made = attend(turned_b[n], keys, values, scales[1])
        attn[:, (wide + n) * LANES : (wide + n + 1) * LANES] = made.astype(jnp.bfloat16)
    split = wide * LANES
    band = resid.shape[0]
    for p in tp_peers + [tp]:
        at = pl.ds(pl.multiple_of(p * band, band), band)
        part[p] = (
            jnp.dot(attn[at, 0:split], out_a[...], preferred_element_type=f32)
            + jnp.dot(attn[at, split:], out_b[...], preferred_element_type=f32)
        ).astype(jnp.bfloat16)
    for i, p in enumerate(tp_peers):
        copy = remote(part.at[p], part_in.at[tp], s_part.at[i], r_part.at[tp], {"tp": p})
        copy.start()
        started.append(copy)
    for i in range(1, outer - 1):
        forward(1, i)
    sums = resid[...].astype(f32) + part[tp].astype(f32)
    for p in tp_peers:
        arrive(part_in.at[p], r_part.at[p])
        sums = sums + part_in[p].astype(f32)
    mid[...] = sums.astype(jnp.bfloat16)
    midf = mid[...].astype(f32)
    norm = lax.rsqrt(jnp.mean(midf * midf, axis=-1, keepdims=True) + EPS)
    normed[...] = (midf * norm * norm_gain[...]).astype(jnp.bfloat16)
    for i in range(outer - 1):
        forward(2, i)
    settle(1)
    settle(2)
    for copy in own[1:]:
        copy.wait()
    for copy in started:
        copy.wait_send()


def front(kv, q_a, q_b, table, gains, resid, norm_gain, out_a, out_b, up, down, total, lanes):
    outer = total // INNER
    units = up.shape[1] // outer
    kind = jnp.bfloat16
    scales = ((LANES // 2) ** (-0.5), LANES ** (-0.5))
    features = q_a.shape[1] + q_b.shape[1]
    vmem = pl.BlockSpec(memory_space=pltpu.VMEM)
    sems = pltpu.SemaphoreType.DMA
    return pl.pallas_call(
        lambda *refs: front_kernel(outer, lanes, scales, *refs),
        out_shape=(
            jax.ShapeDtypeStruct((up.shape[0] * total, units), up.dtype),
            jax.ShapeDtypeStruct((units, down.shape[1] * total), down.dtype),
            jax.ShapeDtypeStruct(resid.shape, resid.dtype),
            jax.ShapeDtypeStruct(resid.shape, resid.dtype),
        ),
        in_specs=[vmem] * 11,
        out_specs=(vmem,) * 4,
        scratch_shapes=[
            pltpu.VMEM(kv.shape, kind),
            pltpu.VMEM((total,) + kv.shape, kind),
            pltpu.VMEM((q_a.shape[0], features), kind),
            pltpu.VMEM((lanes,) + resid.shape, kind),
            pltpu.VMEM((lanes,) + resid.shape, kind),
            sems((3, total)),
            sems((3, total)),
            sems((3,)),
            sems((lanes - 1,)),
            sems((lanes,)),
        ],
        compiler_params=pltpu.CompilerParams(
            collective_id=0, has_side_effects=True, vmem_limit_bytes=56 * 1024 * 1024
        ),
        name="front",
    )(kv, q_a, q_b, table, gains, resid, norm_gain, out_a, out_b, up, down)


def tail_kernel(
    outer,
    sides,
    normed,
    mid,
    up,
    down,
    out,
    tokens,
    core_out,
    core_in,
    side_out,
    side_in,
    keep,
    ring_out,
    ring_in,
    s_tok,
    r_tok,
    s_core,
    r_core,
    s_side,
    r_side,
    s_ring,
    r_ring,
):
    sp = lax.axis_index("sp")
    tp = lax.axis_index("tp")
    z = sp // INNER
    y = sp % INNER
    x = tp // INNER
    c = tp % INNER
    lanes = sides * INNER
    rows, width = mid.shape
    f32 = jnp.float32
    z_peers = peers_of(z, outer)
    x_peers = peers_of(x, sides)
    other = 1 - c
    greet(
        [{"sp": p * INNER + y} for p in z_peers]
        + [{"tp": p * INNER + c} for p in x_peers]
        + [{"tp": x * INNER + other}]
    )
    started = []

    def ship(src, dst, send, recv, target):
        copy = remote(src, dst, send, recv, target)
        copy.start()
        started.append(copy)

    sent = [0]

    def pass_on(src, k, lane, target):
        ship(src, tokens.at[k, lane], s_tok.at[sent[0]], r_tok.at[k, lane], target)
        sent[0] += 1

    for k, p in enumerate(z_peers):
        pass_on(normed, k + 1, tp, {"sp": p * INNER + y})
    for p in x_peers:
        pass_on(normed, 0, tp, {"tp": p * INNER + c})
    pass_on(normed, 0, tp, {"tp": x * INNER + other})
    tokens[0, tp] = normed[...]

    def spread(k):
        arrive(tokens.at[k, tp], r_tok.at[k, tp])
        for p in x_peers:
            pass_on(tokens.at[k, tp], k, tp, {"tp": p * INNER + c})
        pass_on(tokens.at[k, tp], k, tp, {"tp": x * INNER + other})

    def relay(k):
        for p in x_peers:
            lane = p * INNER + c
            arrive(tokens.at[k, lane], r_tok.at[k, lane])
            pass_on(tokens.at[k, lane], k, lane, {"tp": x * INNER + other})

    def complete(k):
        value = keep[k]
        for d in range(sides - 1):
            arrive(side_in.at[k, d], r_side.at[k, d])
            value = value + side_in[k, d].astype(f32)
        if k == 0:
            keep[0] = value
            return
        ring_out[k - 1] = value.astype(jnp.bfloat16)
        target = {"sp": z_peers[k - 1] * INNER + y}
        ship(ring_out.at[k - 1], ring_in.at[k - 1], s_ring.at[k - 1], r_ring.at[k - 1], target)

    for k in range(outer):
        relay(k)
        if k + 1 < outer:
            spread(k + 1)
        for p in range(sides):
            lane = p * INNER + other
            arrive(tokens.at[k, lane], r_tok.at[k, lane])
        block = tokens[k].reshape(lanes * rows, width)
        made = jnp.maximum(jnp.dot(block, up[...], preferred_element_type=f32), 0.0)
        hidden = (made * made).astype(jnp.bfloat16)
        sums = jnp.dot(hidden, down[...], preferred_element_type=f32)
        sums = sums.reshape(sides, INNER, rows, width)
        mine = jnp.where(c == 0, sums[:, 0], sums[:, 1])
        core_out[k] = jnp.where(c == 0, sums[:, 1], sums[:, 0]).astype(jnp.bfloat16)
        ship(core_out.at[k], core_in.at[k], s_core.at[k], r_core.at[k], {"tp": x * INNER + other})
        if k >= 1:
            complete(k - 1)
        arrive(core_in.at[k], r_core.at[k])
        mine = mine + core_in[k].astype(f32)
        side_out[k] = mine.astype(jnp.bfloat16)
        held = mine[0]
        for n in range(1, sides):
            held = jnp.where(x == n, mine[n], held)
        keep[k] = held
        for d, p in enumerate(x_peers):
            ship(
                side_out.at[k, p],
                side_in.at[k, d],
                s_side.at[k, d],
                r_side.at[k, d],
                {"tp": p * INNER + c},
            )
    complete(outer - 1)
    value = mid[...].astype(f32) + keep[0]
    for k in range(outer - 1):
        arrive(ring_in.at[k], r_ring.at[k])
        value = value + ring_in[k].astype(f32)
    out[...] = value.astype(out.dtype)
    for copy in started:
        copy.wait_send()


def tail(normed, mid, up, down, total, lanes):
    outer = total // INNER
    sides = lanes // INNER
    rows, width = mid.shape
    kind = jnp.bfloat16
    vmem = pl.BlockSpec(memory_space=pltpu.VMEM)
    sems = pltpu.SemaphoreType.DMA
    moves = outer - 1 + outer * (2 * sides - 1)
    near = sides - 1
    far = outer - 1
    return pl.pallas_call(
        lambda *refs: tail_kernel(outer, sides, *refs),
        out_shape=jax.ShapeDtypeStruct(mid.shape, mid.dtype),
        in_specs=[vmem] * 4,
        out_specs=vmem,
        scratch_shapes=[
            pltpu.VMEM((outer, lanes, rows, width), kind),
            pltpu.VMEM((outer, sides, rows, width), kind),
            pltpu.VMEM((outer, sides, rows, width), kind),
            pltpu.VMEM((outer, sides, rows, width), kind),
            pltpu.VMEM((outer, near, rows, width), kind),
            pltpu.VMEM((outer, rows, width), jnp.float32),
            pltpu.VMEM((far, rows, width), kind),
            pltpu.VMEM((far, rows, width), kind),
            sems((moves,)),
            sems((outer, lanes)),
            sems((outer,)),
            sems((outer,)),
            sems((outer, near)),
            sems((outer, near)),
            sems((far,)),
            sems((far,)),
        ],
        compiler_params=pltpu.CompilerParams(
            collective_id=1, has_side_effects=True, vmem_limit_bytes=56 * 1024 * 1024
        ),
        name="tail",
    )(normed, mid, up, down)


def turning_table(places, width, repeat):
    quarter = width // 4
    index = jnp.arange(width * repeat, dtype=jnp.int32) % width
    freqs = 10000.0 ** (-(2.0 * (index % quarter).astype(jnp.float32)) / (width // 2))
    grid = jnp.where(index < width // 2, places[:, None] // GRID_W, places[:, None] % GRID_W)
    angles = grid.astype(jnp.float32) * freqs
    return [jnp.cos(angles), jnp.sin(angles)]


def kernel_local(
    total,
    lanes,
    resid,
    query_a,
    key_a,
    value_a,
    query_b,
    key_b,
    value_b,
    gain_qa,
    gain_ka,
    gain_qb,
    gain_kb,
    w_out_a,
    w_out_b,
    norm_gain,
    w_up,
    w_down,
):
    count = query_a.shape[0]
    places = lax.axis_index("sp") * count + jnp.arange(count, dtype=jnp.int32)
    kv = jnp.concatenate([key_b, value_b, key_a, value_a], axis=1)
    table = jnp.concatenate(
        turning_table(places, gain_qb.shape[0], 1) + turning_table(places, gain_qa.shape[0], 2),
        axis=1,
    )
    gains = jnp.stack([gain_qb, gain_kb, jnp.tile(gain_qa, 2), jnp.tile(gain_ka, 2)])
    up, down, mid, normed = front(
        kv,
        query_a,
        query_b,
        table,
        gains,
        resid,
        norm_gain.reshape(1, -1),
        w_out_a,
        w_out_b,
        w_up,
        w_down,
        total,
        lanes,
    )
    return tail(normed, mid, up, down, total, lanes)


def fits(total, lanes, args):
    outer = total // INNER
    sides = lanes // INNER
    if total % INNER or lanes % INNER or outer < 2 or sides < 2:
        return False
    if outer & (outer - 1) or sides & (sides - 1):
        return False
    key_a, key_b, gain_a, gain_b = args[2], args[5], args[7], args[9]
    if 2 * gain_a.shape[0] != LANES or gain_b.shape[0] != LANES:
        return False
    if key_a.shape[1] != lanes * LANES // 2 or key_b.shape[1] != lanes * LANES:
        return False
    if args[1].shape[1] % (lanes * LANES) or args[4].shape[1] % (lanes * LANES):
        return False
    w_up, w_down = args[-2], args[-1]
    units = w_up.shape[1] // lanes // outer
    rows = w_up.shape[0] // total
    cols = w_down.shape[1] // total
    small = units * w_up.shape[0] <= 2**20 and args[0].shape[0] <= 2**11
    return units % LANES == 0 and rows % 16 == 0 and cols % LANES == 0 and small


def sharded(inside, mesh):
    return jax.shard_map(
        inside,
        mesh=mesh,
        in_specs=(
            P(("sp", "tp"), None),
            P("sp", "tp"),
            P("sp", "tp"),
            P("sp", "tp"),
            P("sp", "tp"),
            P("sp", "tp"),
            P("sp", "tp"),
            P(),
            P(),
            P(),
            P(),
            P("tp", None),
            P("tp", None),
            P(),
            P("sp", "tp"),
            P("tp", "sp"),
        ),
        out_specs=P(("sp", "tp"), None),
        check_vma=False,
    )


def solution(mesh):
    total = mesh.shape["sp"]
    lanes = mesh.shape["tp"]

    def run(*args):
        inside = local
        if fits(total, lanes, args):
            inside = lambda *shards: kernel_local(total, lanes, *shards)
        return sharded(inside, mesh)(*args)

    return run
```

```python
import math

import jax
import jax.numpy as jnp
from jax import lax
from jax.experimental import pallas as pl
from jax.experimental.pallas import tpu as pltpu
from jax.sharding import PartitionSpec as P

GRID_W = 64


EPS = 1e-06


def norm_rope(values, gain, places):
    width = gain.shape[0]
    count = values.shape[0]
    flat = values.astype(jnp.float32).reshape(count, -1, width)
    flat = flat * lax.rsqrt(jnp.mean(flat * flat, axis=-1, keepdims=True) + EPS) * gain
    grid_rows = (places // GRID_W).astype(jnp.float32)
    grid_cols = (places % GRID_W).astype(jnp.float32)
    quarter = width // 4
    freqs = 10000.0 ** (-(2.0 * jnp.arange(quarter, dtype=jnp.float32)) / (width // 2))
    ang_r = grid_rows[:, None] * freqs
    ang_c = grid_cols[:, None] * freqs
    angles = jnp.concatenate([ang_r, ang_r, ang_c, ang_c], axis=-1)
    one, two, three, four = jnp.split(flat, 4, axis=-1)
    turned = jnp.concatenate([-two, one, -four, three], axis=-1)
    return (flat * jnp.cos(angles)[:, None, :] + turned * jnp.sin(angles)[:, None, :]).astype(
        jnp.bfloat16
    )


def fold_block(state, queries, key_block, value_block, scale):
    running, total, accum = state
    scores = (
        jnp.einsum("rkgd,pkd->kgrp", queries, key_block, preferred_element_type=jnp.float32) * scale
    )
    newest = jnp.maximum(running, jnp.max(scores, axis=-1))
    factor = jnp.exp(running - newest)
    expo = jnp.exp(scores - newest[..., None])
    total = total * factor + jnp.sum(expo, axis=-1)
    accum = accum * factor[..., None] + jnp.einsum(
        "kgrp,pkd->kgrd", expo.astype(jnp.bfloat16), value_block, preferred_element_type=jnp.float32
    )
    return (newest, total, accum)


def sweep_keys(state, queries, key_piece, value_piece, scale):
    length = key_piece.shape[0]
    block = math.gcd(length, 2048)
    blocks = length // block
    if blocks == 1:
        return fold_block(state, queries, key_piece, value_piece, scale)
    key_blocks = key_piece.reshape((blocks, block) + key_piece.shape[1:])
    value_blocks = value_piece.reshape((blocks, block) + value_piece.shape[1:])

    def advance(carry, pair):
        return (fold_block(carry, queries, pair[0], pair[1], scale), None)

    state, unused = lax.scan(advance, state, (key_blocks, value_blocks))
    return state


def start_state(queries):
    shape = (queries.shape[1], queries.shape[2], queries.shape[0])
    return (
        jnp.full(shape, -1e30, jnp.float32),
        jnp.zeros(shape, jnp.float32),
        jnp.zeros(shape + (queries.shape[3],), jnp.float32),
    )


def finish(state):
    running, total, accum = state
    outputs = accum / total[..., None]
    count = outputs.shape[2]
    return jnp.transpose(outputs, (2, 0, 1, 3)).reshape(count, -1).astype(jnp.bfloat16)


def local(
    resid,
    query_a,
    key_a,
    value_a,
    query_b,
    key_b,
    value_b,
    gain_qa,
    gain_ka,
    gain_qb,
    gain_kb,
    w_out_a,
    w_out_b,
    norm_gain,
    w_up,
    w_down,
):
    count = query_a.shape[0]
    width_a = gain_qa.shape[0]
    width_b = gain_qb.shape[0]
    places = lax.axis_index("sp") * count + jnp.arange(count, dtype=jnp.int32)
    keys_a = norm_rope(key_a, gain_ka, places)
    keys_b = norm_rope(key_b, gain_kb, places)
    heads_kv_a = keys_a.shape[1]
    heads_kv_b = keys_b.shape[1]
    queries_a = norm_rope(query_a, gain_qa, places)
    queries_b = norm_rope(query_b, gain_qb, places)
    queries_a = queries_a.reshape(count, heads_kv_a, queries_a.shape[1] // heads_kv_a, width_a)
    queries_b = queries_b.reshape(count, heads_kv_b, queries_b.shape[1] // heads_kv_b, width_b)
    values_a = value_a.reshape(count, heads_kv_a, width_a)
    values_b = value_b.reshape(count, heads_kv_b, width_b)
    state_a = sweep_keys(
        start_state(queries_a),
        queries_a,
        lax.all_gather(keys_a, "sp", axis=0, tiled=True),
        lax.all_gather(values_a, "sp", axis=0, tiled=True),
        width_a ** (-0.5),
    )
    state_b = sweep_keys(
        start_state(queries_b),
        queries_b,
        lax.all_gather(keys_b, "sp", axis=0, tiled=True),
        lax.all_gather(values_b, "sp", axis=0, tiled=True),
        width_b ** (-0.5),
    )
    attn_a = finish(state_a)
    attn_b = finish(state_b)
    rows_a, rows_b = (
        lax.all_to_all(attn_a, "tp", split_axis=0, concat_axis=1, tiled=True),
        lax.all_to_all(attn_b, "tp", split_axis=0, concat_axis=1, tiled=True),
    )
    whole_a, whole_b = (
        lax.all_gather(w_out_a, "tp", axis=0, tiled=True),
        lax.all_gather(w_out_b, "tp", axis=0, tiled=True),
    )
    proj = jnp.dot(rows_a, whole_a, preferred_element_type=jnp.float32) + jnp.dot(
        rows_b, whole_b, preferred_element_type=jnp.float32
    )
    mid = (resid.astype(jnp.float32) + proj).astype(jnp.bfloat16)
    midf = mid.astype(jnp.float32)
    normed = (
        midf * lax.rsqrt(jnp.mean(midf * midf, axis=-1, keepdims=True) + EPS) * norm_gain
    ).astype(jnp.bfloat16)
    up_whole, down_whole = (
        lax.all_gather(w_up, "sp", axis=0, tiled=True),
        lax.all_gather(w_down, "sp", axis=1, tiled=True),
    )
    hidden = jnp.square(
        jax.nn.relu(
            jnp.dot(
                lax.all_gather(normed, "tp", axis=0, tiled=True),
                up_whole,
                preferred_element_type=jnp.float32,
            )
        )
    ).astype(jnp.bfloat16)
    mixed = lax.psum_scatter(
        jnp.dot(hidden, down_whole, preferred_element_type=jnp.float32).astype(jnp.bfloat16),
        "tp",
        scatter_dimension=0,
        tiled=True,
    ).astype(jnp.float32)
    return (midf + mixed).astype(jnp.bfloat16)


MESH = pl.DeviceIdType.MESH
INNER = 2
LANES = 128


def remote(src, dst, send, recv, target):
    return pltpu.make_async_remote_copy(
        src_ref=src,
        dst_ref=dst,
        send_sem=send,
        recv_sem=recv,
        device_id=target,
        device_id_type=MESH,
    )


def greet(targets):
    barrier = pltpu.get_barrier_semaphore()
    for target in targets:
        pl.semaphore_signal(barrier, inc=1, device_id=target, device_id_type=MESH)
    pl.semaphore_wait(barrier, len(targets))


def flip(place, k):
    bit = 1
    while bit <= k:
        if k & bit:
            place = place + bit - 2 * bit * lax.rem(place // bit, 2)
        bit *= 2
    return place


def peers_of(place, count):
    return [flip(place, k) for k in range(count - 1, 0, -1)]


def arrive(dst, sem):
    pltpu.make_async_copy(dst, dst, sem).wait()


def front_kernel(
    outer,
    lanes,
    scales,
    k_a,
    v_a,
    k_b,
    v_b,
    q_a,
    q_b,
    cos_a,
    sin_a,
    cos_b,
    sin_b,
    gain_qa,
    gain_ka,
    gain_qb,
    gain_kb,
    resid,
    norm_gain,
    out_a,
    out_b,
    up,
    down,
    up_all,
    down_all,
    mid,
    normed,
    kv,
    kv_all,
    attn,
    part,
    part_in,
    send,
    recv,
    here,
    s_part,
    r_part,
):
    f32 = jnp.float32
    sp = lax.axis_index("sp")
    tp = lax.axis_index("tp")
    z = sp // INNER
    y = sp % INNER
    rows = up.shape[0]
    cols = down.shape[1]
    units = up_all.shape[1]
    count = q_a.shape[0]
    total = outer * INNER
    z_peers = peers_of(z, outer)
    y_peers = peers_of(y, INNER)
    tp_peers = peers_of(tp, lanes)
    greet(
        [{"sp": p * INNER + y} for p in z_peers]
        + [{"sp": z * INNER + p} for p in y_peers]
        + [{"tp": p} for p in tp_peers]
    )
    lane = lax.broadcasted_iota(jnp.int32, (count, LANES), 1)
    low = lane < LANES // 2

    def spin(value, quarter):
        even = lax.rem(lane // quarter, 2) == 0
        ahead = pltpu.roll(value, LANES - quarter, 1)
        behind = pltpu.roll(value, quarter, 1)
        return jnp.where(even, -ahead, behind)

    def turn_b(raw, gain):
        value = raw.astype(f32)
        value = value * lax.rsqrt(jnp.mean(value * value, axis=-1, keepdims=True) + EPS) * gain
        return value * cos_b[...] + spin(value, LANES // 4) * sin_b[...]

    def turn_a(raw, gain):
        value = raw.astype(f32)
        square = value * value
        first = jnp.sum(jnp.where(low, square, 0.0), axis=-1, keepdims=True)
        second = jnp.sum(jnp.where(low, 0.0, square), axis=-1, keepdims=True)
        mean = jnp.where(low, first, second) * (2.0 / LANES)
        value = value * lax.rsqrt(mean + EPS) * gain
        return value * cos_a[...] + spin(value, LANES // 8) * sin_a[...]

    def twice(ref):
        return jnp.concatenate([ref[...], ref[...]], axis=1)

    raw = jnp.concatenate([k_a[...].astype(f32), v_a[...].astype(f32)], axis=1)
    keys = turn_a(raw, twice(gain_ka))
    kv[:, 2 * LANES : 3 * LANES] = jnp.where(low, keys, raw).astype(jnp.bfloat16)
    kv[:, 0:LANES] = turn_b(k_b[...], gain_kb[...]).astype(jnp.bfloat16)
    kv[:, LANES : 2 * LANES] = v_b[...]

    def piece(m, target):
        at = pl.ds(pl.multiple_of(target * units, units), units)
        if m == 0:
            return kv
        return up.at[:, at] if m == 1 else down.at[at, :]

    def place(m, source):
        if m == 0:
            return kv_all.at[source]
        if m == 1:
            return up_all.at[pl.ds(pl.multiple_of(source * rows, rows), rows), :]
        return down_all.at[:, pl.ds(pl.multiple_of(source * cols, cols), cols)]

    started = []

    def ship(m, slot, src, source, target):
        copy = remote(src, place(m, source), send.at[m, slot], recv.at[m, source], target)
        copy.start()
        started.append(copy)

    def open_z(m):
        for i, p in enumerate(z_peers):
            ship(m, i, piece(m, p), sp, {"sp": p * INNER + y})

    def open_y(m):
        for i, p in enumerate(y_peers):
            ship(m, outer - 1 + i, piece(m, z), sp, {"sp": z * INNER + p})

    def forward(m, i):
        source = z_peers[i] * INNER + y
        arrive(place(m, source), recv.at[m, source])
        for n, p in enumerate(y_peers):
            slot = outer - 1 + (i + 1) * (INNER - 1) + n
            ship(m, slot, place(m, source), source, {"sp": z * INNER + p})

    def settle(m):
        for p in y_peers:
            for zs in range(outer):
                source = zs * INNER + p
                arrive(place(m, source), recv.at[m, source])

    own = []
    open_z(0)
    open_y(0)
    for m in (1, 2):
        open_z(m)
    open_y(1)
    for m in range(3):
        copy = pltpu.make_async_copy(piece(m, z), place(m, sp), here.at[m])
        copy.start()
        own.append(copy)
    wide = q_a.shape[1] // LANES
    tall = q_b.shape[1] // LANES
    turned_a = []
    turned_b = []
    for n in range(wide):
        value = turn_a(q_a[:, n * LANES : (n + 1) * LANES], twice(gain_qa))
        other = pltpu.roll(value, LANES // 2, 1)
        for v in (value, other):
            turned_a.append(jnp.where(low, v, 0.0).astype(jnp.bfloat16))
    for n in range(tall):
        value = turn_b(q_b[:, n * LANES : (n + 1) * LANES], gain_qb[...])
        turned_b.append(value.astype(jnp.bfloat16))
    for i in range(outer - 1):
        forward(0, i)
    open_y(2)
    own[0].wait()
    settle(0)

    def attend(query, keys, values, scale):
        scores = lax.dot_general(
            query, keys, (((1,), (1,)), ((), ())), preferred_element_type=f32
        )
        scores = scores * scale
        expo = jnp.exp(scores - jnp.max(scores, axis=-1, keepdims=True))
        summed = jnp.dot(expo.astype(jnp.bfloat16), values, preferred_element_type=f32)
        return summed / jnp.sum(expo, axis=-1, keepdims=True)

    both = kv_all[:, :, 2 * LANES : 3 * LANES].reshape(total * count, LANES)
    for n in range(wide):
        first = attend(turned_a[2 * n], both, both, scales[0])
        second = attend(turned_a[2 * n + 1], both, both, scales[0])
        pair = jnp.where(low, pltpu.roll(first, LANES // 2, 1), second)
        attn[:, n * LANES : (n + 1) * LANES] = pair.astype(jnp.bfloat16)
    forward(1, 0)
    keys = kv_all[:, :, 0:LANES].reshape(total * count, LANES)
    values = kv_all[:, :, LANES : 2 * LANES].reshape(total * count, LANES)
    for n in range(tall):
        made = attend(turned_b[n], keys, values, scales[1])
        attn[:, (wide + n) * LANES : (wide + n + 1) * LANES] = made.astype(jnp.bfloat16)
    split = wide * LANES
    band = resid.shape[0]
    for p in tp_peers + [tp]:
        at = pl.ds(pl.multiple_of(p * band, band), band)
        part[p] = (
            jnp.dot(attn[at, 0:split], out_a[...], preferred_element_type=f32)
            + jnp.dot(attn[at, split:], out_b[...], preferred_element_type=f32)
        ).astype(jnp.bfloat16)
    for i, p in enumerate(tp_peers):
        copy = remote(part.at[p], part_in.at[tp], s_part.at[i], r_part.at[tp], {"tp": p})
        copy.start()
        started.append(copy)
    for i in range(1, outer - 1):
        forward(1, i)
    sums = resid[...].astype(f32) + part[tp].astype(f32)
    for p in tp_peers:
        arrive(part_in.at[p], r_part.at[p])
        sums = sums + part_in[p].astype(f32)
    mid[...] = sums.astype(jnp.bfloat16)
    midf = mid[...].astype(f32)
    norm = lax.rsqrt(jnp.mean(midf * midf, axis=-1, keepdims=True) + EPS)
    normed[...] = (midf * norm * norm_gain[...]).astype(jnp.bfloat16)
    forward(2, 0)

    def close():
        for i in range(1, outer - 1):
            forward(2, i)
        settle(1)
        settle(2)
        for copy in own[1:]:
            copy.wait()

    return close, started


def tail_kernel(
    outer,
    sides,
    close,
    normed,
    mid,
    up,
    down,
    out,
    tokens,
    core_out,
    core_in,
    side_out,
    side_in,
    keep,
    ring_out,
    ring_in,
    s_tok,
    r_tok,
    s_core,
    r_core,
    s_side,
    r_side,
    s_ring,
    r_ring,
):
    sp = lax.axis_index("sp")
    tp = lax.axis_index("tp")
    z = sp // INNER
    y = sp % INNER
    x = tp // INNER
    c = tp % INNER
    lanes = sides * INNER
    rows, width = mid.shape
    f32 = jnp.float32
    z_peers = peers_of(z, outer)
    x_peers = peers_of(x, sides)
    other = 1 - c
    started = []

    def ship(src, dst, send, recv, target):
        copy = remote(src, dst, send, recv, target)
        copy.start()
        started.append(copy)

    sent = [0]

    def pass_on(src, k, lane, target):
        ship(src, tokens.at[k, lane], s_tok.at[sent[0]], r_tok.at[k, lane], target)
        sent[0] += 1

    for k, p in enumerate(z_peers):
        pass_on(normed, k + 1, tp, {"sp": p * INNER + y})
    for p in x_peers:
        pass_on(normed, 0, tp, {"tp": p * INNER + c})
    pass_on(normed, 0, tp, {"tp": x * INNER + other})
    tokens[0, tp] = normed[...]
    close()

    def spread(k):
        arrive(tokens.at[k, tp], r_tok.at[k, tp])
        for p in x_peers:
            pass_on(tokens.at[k, tp], k, tp, {"tp": p * INNER + c})
        pass_on(tokens.at[k, tp], k, tp, {"tp": x * INNER + other})

    def relay(k):
        for p in x_peers:
            lane = p * INNER + c
            arrive(tokens.at[k, lane], r_tok.at[k, lane])
            pass_on(tokens.at[k, lane], k, lane, {"tp": x * INNER + other})

    def complete(k):
        value = keep[k]
        for d in range(sides - 1):
            arrive(side_in.at[k, d], r_side.at[k, d])
            value = value + side_in[k, d].astype(f32)
        if k == 0:
            keep[0] = value
            return
        ring_out[k - 1] = value.astype(jnp.bfloat16)
        target = {"sp": z_peers[k - 1] * INNER + y}
        ship(ring_out.at[k - 1], ring_in.at[k - 1], s_ring.at[k - 1], r_ring.at[k - 1], target)

    for k in range(outer):
        relay(k)
        if k + 1 < outer:
            spread(k + 1)
        for p in range(sides):
            lane = p * INNER + other
            arrive(tokens.at[k, lane], r_tok.at[k, lane])
        block = tokens[k].reshape(lanes * rows, width)
        made = jnp.maximum(jnp.dot(block, up[...], preferred_element_type=f32), 0.0)
        hidden = (made * made).astype(jnp.bfloat16)
        sums = jnp.dot(hidden, down[...], preferred_element_type=f32)
        sums = sums.reshape(sides, INNER, rows, width)
        mine = jnp.where(c == 0, sums[:, 0], sums[:, 1])
        core_out[k] = jnp.where(c == 0, sums[:, 1], sums[:, 0]).astype(jnp.bfloat16)
        ship(core_out.at[k], core_in.at[k], s_core.at[k], r_core.at[k], {"tp": x * INNER + other})
        if k >= 1:
            complete(k - 1)
        arrive(core_in.at[k], r_core.at[k])
        mine = mine + core_in[k].astype(f32)
        side_out[k] = mine.astype(jnp.bfloat16)
        held = mine[0]
        for n in range(1, sides):
            held = jnp.where(x == n, mine[n], held)
        keep[k] = held
        for d, p in enumerate(x_peers):
            ship(
                side_out.at[k, p],
                side_in.at[k, d],
                s_side.at[k, d],
                r_side.at[k, d],
                {"tp": p * INNER + c},
            )
    complete(outer - 1)
    value = mid[...].astype(f32) + keep[0]
    for k in range(outer - 1):
        arrive(ring_in.at[k], r_ring.at[k])
        value = value + ring_in[k].astype(f32)
    out[...] = value.astype(out.dtype)
    for copy in started:
        copy.wait_send()


def layer_kernel(outer, lanes, scales, *refs):
    operands, out, carried = refs[:20], refs[20], refs[21:25]
    close, started = front_kernel(outer, lanes, scales, *operands, *carried, *refs[25:35])
    up_all, down_all, mid, normed = carried
    sides = lanes // INNER
    tail_kernel(outer, sides, close, normed, mid, up_all, down_all, out, *refs[35:])
    for copy in started:
        copy.wait_send()


def layer(operands, total, lanes):
    count = operands[0].shape[0]
    q_a, q_b, resid = operands[4], operands[5], operands[14]
    up, down = operands[18], operands[19]
    outer = total // INNER
    sides = lanes // INNER
    rows, width = resid.shape
    units = up.shape[1] // outer
    kind = jnp.bfloat16
    scales = ((LANES // 2) ** (-0.5), LANES ** (-0.5))
    features = q_a.shape[1] + q_b.shape[1]
    vmem = pl.BlockSpec(memory_space=pltpu.VMEM)
    sems = pltpu.SemaphoreType.DMA
    moves = outer - 1 + outer * (2 * sides - 1)
    near = sides - 1
    far = outer - 1
    carried = [
        pltpu.VMEM((up.shape[0] * total, units), kind),
        pltpu.VMEM((units, down.shape[1] * total), kind),
        pltpu.VMEM(resid.shape, kind),
        pltpu.VMEM(resid.shape, kind),
    ]
    first = [
        pltpu.VMEM((count, 3 * LANES), kind),
        pltpu.VMEM((total, count, 3 * LANES), kind),
        pltpu.VMEM((count, features), kind),
        pltpu.VMEM((lanes, rows, width), kind),
        pltpu.VMEM((lanes, rows, width), kind),
        sems((3, total)),
        sems((3, total)),
        sems((3,)),
        sems((lanes - 1,)),
        sems((lanes,)),
    ]
    second = [
        pltpu.VMEM((outer, lanes, rows, width), kind),
        pltpu.VMEM((outer, sides, rows, width), kind),
        pltpu.VMEM((outer, sides, rows, width), kind),
        pltpu.VMEM((outer, sides, rows, width), kind),
        pltpu.VMEM((outer, near, rows, width), kind),
        pltpu.VMEM((outer, rows, width), jnp.float32),
        pltpu.VMEM((far, rows, width), kind),
        pltpu.VMEM((far, rows, width), kind),
        sems((moves,)),
        sems((outer, lanes)),
        sems((outer,)),
        sems((outer,)),
        sems((outer, near)),
        sems((outer, near)),
        sems((far,)),
        sems((far,)),
    ]
    return pl.pallas_call(
        lambda *refs: layer_kernel(outer, lanes, scales, *refs),
        out_shape=jax.ShapeDtypeStruct(resid.shape, resid.dtype),
        in_specs=[vmem] * 20,
        out_specs=vmem,
        scratch_shapes=carried + first + second,
        compiler_params=pltpu.CompilerParams(
            collective_id=0, has_side_effects=True, vmem_limit_bytes=60 * 1024 * 1024
        ),
        name="layer",
    )(*operands)


def turning_table(places, width, repeat):
    quarter = width // 4
    index = jnp.arange(width * repeat, dtype=jnp.int32) % width
    freqs = 10000.0 ** (-(2.0 * (index % quarter).astype(jnp.float32)) / (width // 2))
    grid = jnp.where(index < width // 2, places[:, None] // GRID_W, places[:, None] % GRID_W)
    angles = grid.astype(jnp.float32) * freqs
    return [jnp.cos(angles), jnp.sin(angles)]


def kernel_local(
    total,
    lanes,
    resid,
    query_a,
    key_a,
    value_a,
    query_b,
    key_b,
    value_b,
    gain_qa,
    gain_ka,
    gain_qb,
    gain_kb,
    w_out_a,
    w_out_b,
    norm_gain,
    w_up,
    w_down,
):
    count = query_a.shape[0]
    places = lax.axis_index("sp") * count + jnp.arange(count, dtype=jnp.int32)
    cos_a, sin_a = turning_table(places, gain_qa.shape[0], 2)
    cos_b, sin_b = turning_table(places, gain_qb.shape[0], 1)
    gains = [g.reshape(1, -1) for g in (gain_qa, gain_ka, gain_qb, gain_kb)]
    operands = [key_a, value_a, key_b, value_b, query_a, query_b, cos_a, sin_a, cos_b, sin_b]
    operands += gains + [resid, norm_gain.reshape(1, -1), w_out_a, w_out_b, w_up, w_down]
    return layer(operands, total, lanes)


def fits(total, lanes, args):
    outer = total // INNER
    sides = lanes // INNER
    if total % INNER or lanes % INNER or outer < 2 or sides < 2:
        return False
    if outer & (outer - 1) or sides & (sides - 1):
        return False
    key_a, key_b, gain_a, gain_b = args[2], args[5], args[7], args[9]
    if 2 * gain_a.shape[0] != LANES or gain_b.shape[0] != LANES:
        return False
    if key_a.shape[1] != lanes * LANES // 2 or key_b.shape[1] != lanes * LANES:
        return False
    if args[1].shape[1] % (lanes * LANES) or args[4].shape[1] % (lanes * LANES):
        return False
    w_up, w_down = args[-2], args[-1]
    units = w_up.shape[1] // lanes // outer
    rows = w_up.shape[0] // total
    cols = w_down.shape[1] // total
    small = units * w_up.shape[0] <= 2**20 and args[0].shape[0] <= 2**11
    return units % LANES == 0 and rows % 16 == 0 and cols % LANES == 0 and small


def sharded(inside, mesh):
    return jax.shard_map(
        inside,
        mesh=mesh,
        in_specs=(
            P(("sp", "tp"), None),
            P("sp", "tp"),
            P("sp", "tp"),
            P("sp", "tp"),
            P("sp", "tp"),
            P("sp", "tp"),
            P("sp", "tp"),
            P(),
            P(),
            P(),
            P(),
            P("tp", None),
            P("tp", None),
            P(),
            P("sp", "tp"),
            P("tp", "sp"),
        ),
        out_specs=P(("sp", "tp"), None),
        check_vma=False,
    )


def solution(mesh):
    total = mesh.shape["sp"]
    lanes = mesh.shape["tp"]

    def run(*args):
        inside = local
        if fits(total, lanes, args):
            inside = lambda *shards: kernel_local(total, lanes, *shards)
        return sharded(inside, mesh)(*args)

    return run
```
